32 devices in a mesh: fs: 4 (over z), tp: 8 (over y, x, core).
Axes of the slice: x: 2, y: 2, z: 4, core: 2. Of those that a mesh axis runs over, the one named last changes fastest.
Arguments:
- inputs: bfloat16 [1024, 2016], P('fs'), may hold values from -6 to 6
- pre_act: bfloat16 [1024, 4032], P('fs', 'tp'), may hold values from -6 to 6
- cotangent: bfloat16 [1024, 2016], P('fs'), may hold values from -6 to 6
- w_up: bfloat16 [2016, 4032], P('fs', 'tp'), may hold values from -0.125 to 0.125
- w_down: bfloat16 [4032, 2016], P('tp', 'fs'), may hold values from -0.09375 to 0.09375
Outputs:
- grad_input: bfloat16 [1024, 2016], P('fs')
- grad_up: float32 [2016, 4032], P('fs', 'tp')
- grad_down: float32 [4032, 2016], P('tp', 'fs')
The draws below stay inside these ranges and needn't reach their ends.
All inputs are finite; a program needn't handle non-finite values.
Results may differ from the reference program's by a relative error of at most 0.017.
Values may be sent and summed in bfloat16 or wider, within the bound.
No kernel may reach another device: no remote copies, remote signals or barrier semaphores. Data moves between devices by JAX's collectives and lax.ppermute only.
A program may use at most 64 MiB of HBM per device.

```python
import jax
import jax.numpy as jnp
from jax import lax

D = 2016
FF = 4032
TOKENS = 1024
N_TP = 8


def strengthened(entries, rng, source, target, blocks, factor):
    def block_of(position):
        return (jnp.arange(entries.shape[position]) // (entries.shape[position] // blocks)).reshape((-1,) + (1,) * (entries.ndim - 1 - position))

    one_side = jax.random.permutation(rng, blocks)[block_of(target)]
    far = (block_of(target) + blocks // 2) % blocks
    return jnp.where((block_of(source) == one_side) | (block_of(source) == far), factor * entries, entries)


def block_levels(stream_key, shape, split, least, largest):
    def one(axis_at, shards_of):
        steps = jax.random.uniform(jax.random.fold_in(jax.random.fold_in(stream_key, 6), axis_at), (shards_of,), jnp.float32, least / len(split), largest / len(split))
        return jnp.repeat(jnp.exp(steps), shape[axis_at] // shards_of).reshape((-1,) + (1,) * (len(shape) - axis_at - 1))

    factor_of = one(*split[0])
    for cut in split[1:]:
        factor_of = factor_of * one(*cut)
    return factor_of


def gaussian(key, extent, spread, limit, cuts=(), dtype=jnp.bfloat16):
    loudness = block_levels(key, extent, cuts, -0.22, 0.18) if cuts else 1.0
    result = jax.random.normal(key, extent, jnp.float32) * spread * loudness
    return jnp.minimum(jnp.maximum(result, -limit), limit).astype(dtype)


def bell_draw_with(stream_key, shape, deviation, most, split, heavy, held_as=jnp.bfloat16):
    result = deviation * jax.random.normal(stream_key, shape, jnp.float32)
    if split:
        result = result * block_levels(stream_key, shape, split, -0.22, 0.18)
    return jnp.clip(strengthened(result, jax.random.fold_in(stream_key, 3), *heavy), -most, most).astype(held_as)


def setup_inputs(seed: int = 0) -> dict:
    key_of = jax.random.split(jax.random.key(seed), 6)
    inputs = bell_draw_with(key_of[0], (TOKENS, D), 1.0, 6.0, ((0, 4),), (0, 1, 4, 2.0))
    pre_act = gaussian(key_of[1], (TOKENS, FF), 1.0, 6.0, ((0, 4), (1, 8)))
    cotangent = bell_draw_with(key_of[2], (TOKENS, D), 1.0, 6.0, ((0, 4),), (0, 1, 4, 2.0))
    w_up = gaussian(key_of[3], (D, FF), D ** -0.5, 0.125, ((0, 4), (1, 8)))
    w_down = gaussian(key_of[4], (FF, D), FF ** -0.5, 0.09375, ((0, 8), (1, 4)))
    return {"inputs": inputs, "pre_act": pre_act, "cotangent": cotangent, "w_up": w_up, "w_down": w_down}


def reference(inputs, pre_act, cotangent, w_up, w_down):
    positive = jnp.maximum(pre_act.astype(jnp.float32), 0.0)
    hidden = (positive * positive).astype(jnp.bfloat16)
    hidden_grad = lax.dot_general(cotangent, w_down, (((1,), (1,)), ((), ())), preferred_element_type=jnp.float32)
    pre_grad = (2.0 * positive * hidden_grad).astype(jnp.bfloat16)
    grad_down = lax.dot_general(hidden, cotangent, (((0,), (0,)), ((), ())), preferred_element_type=jnp.float32)
    grad_up = lax.dot_general(inputs, pre_grad, (((0,), (0,)), ((), ())), preferred_element_type=jnp.float32)
    width = FF // N_TP

    def add_block(index, total):
        start = (index * width).astype(jnp.int32)
        piece_grad = lax.dynamic_slice_in_dim(pre_grad, start, width, 1)
        piece_weight = lax.dynamic_slice_in_dim(w_up, start, width, 1)
        partial_sum = lax.dot_general(piece_grad, piece_weight, (((1,), (1,)), ((), ())), preferred_element_type=jnp.float32).astype(jnp.bfloat16)
        partial_sum = lax.optimization_barrier(partial_sum)
        return total + partial_sum.astype(jnp.float32)

    total = lax.fori_loop(0, N_TP, add_block, jnp.zeros((TOKENS, D), jnp.float32))
    return total.astype(jnp.bfloat16), grad_up, grad_down
```

```python
import jax
import jax.numpy as jnp
from jax import lax
from jax.sharding import PartitionSpec as P

F32, BF16 = jnp.float32, jnp.bfloat16


def dot(a, b, ca, cb):
    return lax.dot_general(a, b, (((ca,), (cb,)), ((), ())), preferred_element_type=F32)


def body(inputs, pre_act, cotangent, w_up, w_down, n_fs, n_tp):
    groups = n_fs // 2
    tokens, width = inputs.shape
    block = width // n_fs
    share = tokens // n_tp
    me = lax.axis_index("fs")
    group, side = me // 2, me % 2
    lane = lax.axis_index("tp")

    sibling = [(p, p ^ 1) for p in range(n_fs)]

    def shift(x, k):
        return lax.ppermute(x, "fs", [(p, (p + 2 * k) % n_fs) for p in range(n_fs)])

    def columns(x, row, rows, k):
        base = 2 * ((group + k) % groups)
        own = lax.dynamic_slice(x, (row, (base + side) * block), (rows, block))
        other = lax.dynamic_slice(x, (row, (base + 1 - side) * block), (rows, block))
        return jnp.concatenate([own, other], axis=1)

    cot_shares = [shift(columns(cotangent, lane * share, share, k), k) for k in range(1, groups)]
    w_down_g = jnp.concatenate([w_down, lax.ppermute(w_down, "fs", sibling)], axis=1)
    cot = [columns(cotangent, 0, tokens, 0)]
    cot += [lax.all_gather(s, "tp", axis=0, tiled=True) for s in cot_shares]

    partial = [dot(c, w_down_g, 1, 1) for c in cot]
    hidden_grad = partial[0]
    for k in range(1, groups):
        hidden_grad = hidden_grad + shift(partial[k].astype(BF16), -k).astype(F32)
    positive = jnp.maximum(pre_act.astype(F32), 0.0)
    pre_grad = [(2.0 * positive * hidden_grad).astype(BF16)]
    pre_grad += [shift(pre_grad[0], k) for k in range(1, groups)]

    acts = [pre_act] + [shift(pre_act, k) for k in range(1, groups)]
    in_shares = [shift(columns(inputs, lane * share, share, k), k) for k in range(1, groups)]
    ins = [columns(inputs, 0, tokens, 0)]
    ins += [lax.all_gather(s, "tp", axis=0, tiled=True) for s in in_shares]
    w_up_g = jnp.concatenate([w_up, lax.ppermute(w_up, "fs", sibling)], axis=0)

    pieces = []
    for k in range(groups):
        terms = dot(pre_grad[k], w_up_g, 1, 1).astype(BF16)
        terms = lax.all_to_all(terms.reshape(n_tp, share, 2 * block), "tp", 0, 0)
        total = jnp.sum(terms.astype(F32), axis=0).astype(BF16)
        pieces.append(total if k == 0 else shift(total, -k))
    pairs = [p[:, :block] for p in pieces], [p[:, block:] for p in pieces]
    ordered = []
    for h in range(groups):
        at = (h - group) % groups
        own, other = pairs[0][0], pairs[1][0]
        for k in range(1, groups):
            own = jnp.where(at == k, pairs[0][k], own)
            other = jnp.where(at == k, pairs[1][k], other)
        ordered += [jnp.where(side == 0, own, other), jnp.where(side == 0, other, own)]
    grad_input = lax.all_gather(jnp.concatenate(ordered, axis=1), "tp", axis=0, tiled=True)

    hidden = []
    for a in acts:
        pos = jnp.maximum(a.astype(F32), 0.0)
        hidden.append((pos * pos).astype(BF16))

    def summed(terms):
        total = terms[0]
        for t in terms[1:]:
            total = total + t
        return total

    down_own = summed([dot(h, c[:, :block], 0, 0) for h, c in zip(hidden, cot)])
    down_other = summed([dot(h, c[:, block:], 0, 0) for h, c in zip(hidden, cot)])
    grad_down = down_own + lax.ppermute(down_other.astype(BF16), "fs", sibling).astype(F32)
    up_own = summed([dot(x[:, :block], p, 0, 0) for x, p in zip(ins, pre_grad)])
    up_other = summed([dot(x[:, block:], p, 0, 0) for x, p in zip(ins, pre_grad)])
    grad_up = up_own + lax.ppermute(up_other.astype(BF16), "fs", sibling).astype(F32)
    return grad_input, grad_up, grad_down


def solution(mesh):
    n_fs, n_tp = mesh.shape["fs"], mesh.shape["tp"]
    in_specs = (P("fs", None), P("fs", "tp"), P("fs", None), P("fs", "tp"), P("tp", "fs"))
    out_specs = (P("fs", None), P("fs", "tp"), P("tp", "fs"))

    def on_device(*args):
        return body(*args, n_fs, n_tp)

    return jax.shard_map(
        on_device, mesh=mesh, in_specs=in_specs, out_specs=out_specs, check_vma=False
    )
```

```python
import jax
import jax.numpy as jnp
from jax import lax
from jax.experimental.layout import Layout, with_layout_constraint
from jax.sharding import PartitionSpec as P

F32, BF16 = jnp.float32, jnp.bfloat16


def dot(a, b, ca, cb):
    return lax.dot_general(a, b, (((ca,), (cb,)), ((), ())), preferred_element_type=F32)


def rows_major(x):
    return with_layout_constraint(x, Layout(major_to_minor=(0, 1)))


def after(x, *deps):
    return lax.optimization_barrier((x, *deps))[0]


def positive(x):
    return jnp.maximum(x.astype(F32), 0.0)


def squared(x):
    return (positive(x) * positive(x)).astype(BF16)


def summed(pairs):
    total = None
    for a, b in pairs:
        term = dot(a, b, 0, 0)
        total = term if total is None else total + term
    return total


def body(inputs, pre_act, cotangent, w_up, w_down, n_fs, n_tp):
    groups = n_fs // 2
    tokens, width = inputs.shape
    block = width // n_fs
    share = tokens // n_tp
    me = lax.axis_index("fs")
    group, side = me // 2, me % 2
    lane = lax.axis_index("tp")
    others = range(1, groups)

    def route(x, k, flip):
        pairs = [(p, (p + 2 * k) % n_fs ^ flip) for p in range(n_fs)]
        return lax.ppermute(x, "fs", pairs)

    def gather(x):
        return lax.all_gather(x, "tp", axis=0, tiled=True)

    def columns(x, row, rows, k, flip):
        at = 2 * ((group + k) % groups) + (side ^ flip)
        return lax.dynamic_slice(x, (row, at * block), (rows, block))

    def both(x, row, rows, k):
        return jnp.concatenate([columns(x, row, rows, k, 0), columns(x, row, rows, k, 1)], axis=1)

    gap = jnp.zeros((share, -2 * block % 128), BF16)
    row = lane * share
    shares = [
        route(jnp.concatenate([both(cotangent, row, share, k), gap, both(inputs, row, share, k)], axis=1), k, 0)
        for k in others
    ]
    w_down_g = jnp.concatenate([w_down, route(w_down, 0, 1)], axis=1)
    w_up_other = route(w_up, 0, 1)
    acts = [route(pre_act, k, 0) for k in others]
    gathered = [gather(s) for s in shares]
    cot = [x[:, : 2 * block] for x in gathered]

    sent = [dot(c, w_down_g, 1, 1).astype(BF16) for c in cot]
    cotangent, inputs, w_up = lax.optimization_barrier((cotangent, inputs, w_up, sent))[:3]
    cot = [both(cotangent, 0, tokens, 0)] + cot
    hidden_grad = lax.optimization_barrier(dot(cot[0], w_down_g, 1, 1))
    for k in others:
        hidden_grad = hidden_grad + route(sent[k - 1], -k, 0).astype(F32)
    pre_grad = [(2.0 * positive(pre_act) * hidden_grad).astype(BF16)]
    pre_grad += [route(pre_grad[0], k, 0) for k in others]
    ins = [both(inputs, 0, tokens, 0)] + [x[:, -2 * block :] for x in gathered]
    w_up_g = jnp.concatenate([w_up, after(w_up_other, pre_grad[0])], axis=0)

    products = []
    for k in range(groups):
        products.append(rows_major(dot(pre_grad[k], w_up_g, 1, 1).astype(BF16)))
    pieces = []
    for k in range(groups):
        terms = after(products[k], pieces[-1]) if k else products[0]
        terms = lax.all_to_all(terms.reshape(n_tp, share, 2 * block), "tp", 0, 0)
        pieces.append(jnp.sum(terms.astype(F32), axis=0).astype(BF16))
    pieces = [pieces[0]] + [route(pieces[k], -k, 0) for k in others]
    ordered = []
    for h in range(groups):
        at = (h - group) % groups
        own, other = pieces[0][:, :block], pieces[0][:, block:]
        for k in others:
            own = jnp.where(at == k, pieces[k][:, :block], own)
            other = jnp.where(at == k, pieces[k][:, block:], other)
        ordered += [jnp.where(side == 0, own, other), jnp.where(side == 0, other, own)]
    grad_input = gather(jnp.concatenate(ordered, axis=1))

    hidden = [squared(a) for a in lax.optimization_barrier(([pre_act] + acts, products[0]))[0]]
    partial = summed([(h, c[:, block:]) for h, c in zip(hidden, cot)]).astype(BF16)
    kept = lax.optimization_barrier(summed([(h, c[:, :block]) for h, c in zip(hidden, cot)]))
    grad_down = kept + route(partial, 0, 1).astype(F32)

    partial = summed([(x[:, block:], p) for x, p in zip(ins, pre_grad)]).astype(BF16)
    kept = lax.optimization_barrier(summed([(x[:, :block], p) for x, p in zip(ins, pre_grad)]))
    received = route(partial, 0, 1)
    grad_up = kept + after(received, grad_input).astype(F32)
    return grad_input, grad_up, grad_down


def solution(mesh):
    n_fs, n_tp = mesh.shape["fs"], mesh.shape["tp"]
    in_specs = (P("fs", None), P("fs", "tp"), P("fs", None), P("fs", "tp"), P("tp", "fs"))
    out_specs = (P("fs", None), P("fs", "tp"), P("tp", "fs"))

    def on_device(*args):
        return body(*args, n_fs, n_tp)

    return jax.shard_map(
        on_device, mesh=mesh, in_specs=in_specs, out_specs=out_specs, check_vma=False
    )
```

```python
import jax
import jax.numpy as jnp
from jax import lax
from jax.experimental.layout import Layout, with_layout_constraint
from jax.sharding import PartitionSpec as P

F32, BF16 = jnp.float32, jnp.bfloat16


def dot(a, b, ca, cb):
    return lax.dot_general(a, b, (((ca,), (cb,)), ((), ())), preferred_element_type=F32)


def rows_major(x):
    return with_layout_constraint(x, Layout(major_to_minor=(0, 1)))


def after(x, *deps):
    return lax.optimization_barrier((x, *deps))[0]


def positive(x):
    return jnp.maximum(x.astype(F32), 0.0)


def squared(x):
    return (positive(x) * positive(x)).astype(BF16)


def summed(pairs):
    total = None
    for a, b in pairs:
        term = dot(a, b, 0, 0)
        total = term if total is None else total + term
    return total


def body(inputs, pre_act, cotangent, w_up, w_down, n_fs, n_tp):
    groups = n_fs // 2
    tokens, width = inputs.shape
    block = width // n_fs
    share = tokens // n_tp
    me = lax.axis_index("fs")
    group, side = me // 2, me % 2
    lane = lax.axis_index("tp")
    others = range(1, groups)

    def route(x, k, flip):
        pairs = [(p, (p + 2 * k) % n_fs ^ flip) for p in range(n_fs)]
        return lax.ppermute(x, "fs", pairs)

    def gather(x):
        return lax.all_gather(x, "tp", axis=0, tiled=True)

    def columns(x, row, rows, k, flip):
        at = 2 * ((group + k) % groups) + (side ^ flip)
        return lax.dynamic_slice(x, (row, at * block), (rows, block))

    def both(x, row, rows, k):
        return jnp.concatenate([columns(x, row, rows, k, 0), columns(x, row, rows, k, 1)], axis=1)

    row = lane * share
    cot_shares = [route(both(cotangent, row, share, k), k, 0) for k in others]
    w_down_other = route(w_down, 0, 1)
    in_shares = [route(both(inputs, row, share, k), k, 0) for k in others]
    cot = [gather(s) for s in cot_shares]
    w_down_g = jnp.concatenate([w_down, w_down_other], axis=1)
    w_up_other = route(w_up, 0, 1)
    acts = [route(pre_act, k, 0) for k in others]

    units = pre_act.shape[1]
    half = (units // 2 + 15) // 16 * 16
    runs = [slice(0, half), slice(half, units)]
    sent = [[dot(c, w_down_g[run], 1, 1).astype(BF16) for c in cot] for run in runs]
    cotangent, inputs, w_up, late = lax.optimization_barrier((cotangent, inputs, w_up, in_shares, sent))[:4]
    cot = [both(cotangent, 0, tokens, 0)] + cot
    pre_grad = []
    for n, run in enumerate(runs):
        hidden_grad = lax.optimization_barrier(dot(cot[0], w_down_g[run], 1, 1))
        for k in others:
            hidden_grad = hidden_grad + route(sent[n][k - 1], -k, 0).astype(F32)
        pre_grad.append((2.0 * positive(pre_act[:, run]) * hidden_grad).astype(BF16))
    pre_grad = [pre_grad] + [[route(p, k, 0) for p in pre_grad] for k in others]
    pre_grad = [jnp.concatenate(p, axis=1) for p in pre_grad]
    ins = [both(inputs, 0, tokens, 0)]
    for x in late:
        x = lax.all_to_all(jnp.broadcast_to(x, (n_tp, *x.shape)), "tp", 0, 0)
        ins.append(x.reshape(tokens, 2 * block))
    w_up_g = jnp.concatenate([w_up, after(w_up_other, pre_grad[0])], axis=0)

    products = []
    for k in range(groups):
        products.append(rows_major(dot(pre_grad[k], w_up_g, 1, 1).astype(BF16)))
    pieces = []
    for k in range(groups):
        halves = products[k].reshape(n_tp // 2, 2, share, 2 * block)
        give = lax.dynamic_index_in_dim(halves, 1 - lane % 2, 1, keepdims=False)
        keep = lax.dynamic_index_in_dim(halves, lane % 2, 1, keepdims=False)
        taken = lax.ppermute(give, "tp", [(t, t ^ 1) for t in range(n_tp)])
        pieces.append((keep.astype(F32) + taken.astype(F32)).astype(BF16))
    same_parity = [list(range(c, n_tp, 2)) for c in (0, 1)]
    terms = after(jnp.concatenate(pieces, axis=1), ins[1:])
    terms = lax.all_to_all(terms, "tp", 0, 0, axis_index_groups=same_parity)
    terms = [terms[:, k * share : (k + 1) * share] for k in range(groups)]
    pieces = [jnp.sum(t.astype(F32), axis=0).astype(BF16) for t in terms]
    pieces = [pieces[0]] + [route(pieces[k], -k, 0) for k in others]
    ordered = []
    for h in range(groups):
        at = (h - group) % groups
        own, other = pieces[0][:, :block], pieces[0][:, block:]
        for k in others:
            own = jnp.where(at == k, pieces[k][:, :block], own)
            other = jnp.where(at == k, pieces[k][:, block:], other)
        ordered += [jnp.where(side == 0, own, other), jnp.where(side == 0, other, own)]
    grad_input = gather(jnp.concatenate(ordered, axis=1))

    hidden = [squared(a) for a in lax.optimization_barrier(([pre_act] + acts, products[0]))[0]]
    partial = summed([(h, c[:, block:]) for h, c in zip(hidden, cot)]).astype(BF16)
    kept = lax.optimization_barrier(summed([(h, c[:, :block]) for h, c in zip(hidden, cot)]))
    grad_down = kept + route(partial, 0, 1).astype(F32)

    partial = summed([(x[:, block:], p) for x, p in zip(ins, pre_grad)]).astype(BF16)
    kept = lax.optimization_barrier(summed([(x[:, :block], p) for x, p in zip(ins, pre_grad)]))
    received = route(partial, 0, 1)
    grad_up = kept + after(received, grad_input).astype(F32)
    return grad_input, grad_up, grad_down


def solution(mesh):
    n_fs, n_tp = mesh.shape["fs"], mesh.shape["tp"]
    in_specs = (P("fs", None), P("fs", "tp"), P("fs", None), P("fs", "tp"), P("tp", "fs"))
    out_specs = (P("fs", None), P("fs", "tp"), P("tp", "fs"))

    def on_device(*args):
        return body(*args, n_fs, n_tp)

    return jax.shard_map(
        on_device, mesh=mesh, in_specs=in_specs, out_specs=out_specs, check_vma=False
    )
```

```python
import jax
import jax.numpy as jnp
from jax import lax
from jax.experimental.layout import Layout, with_layout_constraint
from jax.sharding import PartitionSpec as P

F32, BF16 = jnp.float32, jnp.bfloat16


def dot(a, b, ca, cb):
    return lax.dot_general(a, b, (((ca,), (cb,)), ((), ())), preferred_element_type=F32)


def rows_major(x):
    return with_layout_constraint(x, Layout(major_to_minor=(0, 1)))


def after(x, *deps):
    return lax.optimization_barrier((x, *deps))[0]


def positive(x):
    return jnp.maximum(x.astype(F32), 0.0)


def squared(x):
    return (positive(x) * positive(x)).astype(BF16)


def summed(pairs):
    total = None
    for a, b in pairs:
        term = dot(a, b, 0, 0)
        total = term if total is None else total + term
    return total


def body(inputs, pre_act, cotangent, w_up, w_down, n_fs, n_tp):
    groups = n_fs // 2
    tokens, width = inputs.shape
    block = width // n_fs
    share = tokens // n_tp
    me = lax.axis_index("fs")
    group, side = me // 2, me % 2
    lane = lax.axis_index("tp")
    others = range(1, groups)

    def route(x, k, flip):
        pairs = [(p, (p + 2 * k) % n_fs ^ flip) for p in range(n_fs)]
        return lax.ppermute(x, "fs", pairs)

    def gather(x):
        return lax.all_gather(x, "tp", axis=0, tiled=True)

    def columns(x, row, rows, k, flip):
        at = 2 * ((group + k) % groups) + (side ^ flip)
        return lax.dynamic_slice(x, (row, at * block), (rows, block))

    def both(x, row, rows, k):
        return jnp.concatenate([columns(x, row, rows, k, 0), columns(x, row, rows, k, 1)], axis=1)

    gap = jnp.zeros((share, -2 * block % 128), BF16)
    row = lane * share
    shares = [
        route(jnp.concatenate([both(cotangent, row, share, k), gap, both(inputs, row, share, k)], axis=1), k, 0)
        for k in others
    ]
    w_down_other = route(w_down, 0, 1)
    gathered = [gather(s) for s in shares]
    cot = [x[:, : 2 * block] for x in gathered]
    w_down_g = jnp.concatenate([w_down, w_down_other], axis=1)
    cut = block // 32 * 16
    w_up_parts = [route(w_up[:cut], 0, 1), route(w_up[cut:], 0, 1)]
    acts = [route(pre_act, k, 0) for k in others]

    units = pre_act.shape[1]
    half = (units // 2 + 15) // 16 * 16
    runs = [slice(0, half), slice(half, units)]
    sent = [[dot(c, w_down_g[run], 1, 1).astype(BF16) for c in cot] for run in runs]
    cotangent, inputs, w_up = lax.optimization_barrier((cotangent, inputs, w_up, sent))[:3]
    cot = [both(cotangent, 0, tokens, 0)] + cot
    pre_grad = []
    for n, run in enumerate(runs):
        hidden_grad = lax.optimization_barrier(dot(cot[0], w_down_g[run], 1, 1))
        for k in others:
            hidden_grad = hidden_grad + route(sent[n][k - 1], -k, 0).astype(F32)
        pre_grad.append((2.0 * positive(pre_act[:, run]) * hidden_grad).astype(BF16))
    pre_grad = [pre_grad] + [[route(p, k, 0) for p in pre_grad] for k in others]
    pre_grad = [jnp.concatenate(p, axis=1) for p in pre_grad]
    ins = [both(inputs, 0, tokens, 0)] + [x[:, -2 * block :] for x in gathered]
    w_up_g = jnp.concatenate([w_up, *after(w_up_parts, pre_grad[0])], axis=0)

    products = []
    for k in range(groups):
        products.append(rows_major(dot(pre_grad[k], w_up_g, 1, 1).astype(BF16)))
    pieces = []
    for k in range(groups):
        halves = products[k].reshape(n_tp // 2, 2, share, 2 * block)
        give = lax.dynamic_index_in_dim(halves, 1 - lane % 2, 1, keepdims=False)
        keep = lax.dynamic_index_in_dim(halves, lane % 2, 1, keepdims=False)
        taken = lax.ppermute(give, "tp", [(t, t ^ 1) for t in range(n_tp)])
        pieces.append((keep.astype(F32) + taken.astype(F32)).astype(BF16))
    same_parity = [list(range(c, n_tp, 2)) for c in (0, 1)]
    terms = jnp.concatenate(pieces, axis=1)
    terms = lax.all_to_all(terms, "tp", 0, 0, axis_index_groups=same_parity)
    terms = [terms[:, k * share : (k + 1) * share] for k in range(groups)]
    pieces = [jnp.sum(t.astype(F32), axis=0).astype(BF16) for t in terms]
    pieces = [pieces[0]] + [route(pieces[k], -k, 0) for k in others]
    ordered = []
    for h in range(groups):
        at = (h - group) % groups
        own, other = pieces[0][:, :block], pieces[0][:, block:]
        for k in others:
            own = jnp.where(at == k, pieces[k][:, :block], own)
            other = jnp.where(at == k, pieces[k][:, block:], other)
        ordered += [jnp.where(side == 0, own, other), jnp.where(side == 0, other, own)]
    grad_input = gather(jnp.concatenate(ordered, axis=1))

    hidden = [squared(a) for a in lax.optimization_barrier(([pre_act] + acts, pre_grad[0]))[0]]
    partial = summed([(h, c[:, block:]) for h, c in zip(hidden, cot)]).astype(BF16)
    kept = lax.optimization_barrier(summed([(h, c[:, :block]) for h, c in zip(hidden, cot)]))
    grad_down = kept + route(partial, 0, 1).astype(F32)

    partial = summed([(x[:, block:], p) for x, p in zip(ins, pre_grad)]).astype(BF16)
    kept = lax.optimization_barrier(summed([(x[:, :block], p) for x, p in zip(ins, pre_grad)]))
    received = route(partial, 0, 1)
    grad_up = kept + after(received, grad_input).astype(F32)
    return grad_input, grad_up, grad_down


def solution(mesh):
    n_fs, n_tp = mesh.shape["fs"], mesh.shape["tp"]
    in_specs = (P("fs", None), P("fs", "tp"), P("fs", None), P("fs", "tp"), P("tp", "fs"))
    out_specs = (P("fs", None), P("fs", "tp"), P("tp", "fs"))

    def on_device(*args):
        return body(*args, n_fs, n_tp)

    return jax.shard_map(
        on_device, mesh=mesh, in_specs=in_specs, out_specs=out_specs, check_vma=False
    )
```

```python
import jax
import jax.numpy as jnp
from jax import lax
from jax.experimental.layout import Layout, with_layout_constraint
from jax.sharding import PartitionSpec as P

F32, BF16 = jnp.float32, jnp.bfloat16


def dot(a, b, ca, cb):
    return lax.dot_general(a, b, (((ca,), (cb,)), ((), ())), preferred_element_type=F32)


def rows_major(x):
    return with_layout_constraint(x, Layout(major_to_minor=(0, 1)))


def after(x, *deps):
    return lax.optimization_barrier((x, *deps))[0]


def positive(x):
    return jnp.maximum(x.astype(F32), 0.0)


def squared(x):
    return (positive(x) * positive(x)).astype(BF16)


def summed(pairs):
    total = None
    for a, b in pairs:
        term = dot(a, b, 0, 0)
        total = term if total is None else total + term
    return total


def body(inputs, pre_act, cotangent, w_up, w_down, n_fs, n_tp):
    groups = n_fs // 2
    tokens, width = inputs.shape
    block = width // n_fs
    share = tokens // n_tp
    me = lax.axis_index("fs")
    group, side = me // 2, me % 2
    lane = lax.axis_index("tp")
    others = range(1, groups)

    def route(x, k, flip):
        pairs = [(p, (p + 2 * k) % n_fs ^ flip) for p in range(n_fs)]
        return lax.ppermute(x, "fs", pairs)

    def gather(x):
        return lax.all_gather(x, "tp", axis=0, tiled=True)

    def columns(x, row, rows, k, flip):
        at = 2 * ((group + k) % groups) + (side ^ flip)
        return lax.dynamic_slice(x, (row, at * block), (rows, block))

    def both(x, row, rows, k):
        return jnp.concatenate([columns(x, row, rows, k, 0), columns(x, row, rows, k, 1)], axis=1)

    gap = jnp.zeros((share, -2 * block % 128), BF16)
    row = lane * share
    shares = [
        route(jnp.concatenate([both(cotangent, row, share, k), gap, both(inputs, row, share, k)], axis=1), k, 0)
        for k in others
    ]
    units = pre_act.shape[1]
    half = (units // 2 + 15) // 16 * 16
    runs = [slice(0, half), slice(half, units)]
    w_down_g = [route(w_down[run], 0, 1) for run in runs]
    w_down_g = [jnp.concatenate([w_down[run], w], axis=1) for run, w in zip(runs, w_down_g)]
    gathered = [gather(s) for s in shares]
    cot = [x[:, : 2 * block] for x in gathered]
    cut = block // 32 * 16
    w_up_parts = [route(w_up[:cut], 0, 1)]
    acts = [route(pre_act, k, 0) for k in others]

    sent = []
    for w in w_down_g:
        sent.append([dot(c, w, 1, 1).astype(BF16) for c in cot])
    cotangent, inputs, w_up = lax.optimization_barrier((cotangent, inputs, w_up, sent))[:3]
    w_up_parts.append(route(w_up[cut:], 0, 1))
    cot = [both(cotangent, 0, tokens, 0)] + cot
    pre_grad = []
    for n, run in enumerate(runs):
        hidden_grad = lax.optimization_barrier(dot(cot[0], w_down_g[n], 1, 1))
        for k in others:
            hidden_grad = hidden_grad + route(sent[n][k - 1], -k, 0).astype(F32)
        pre_grad.append((2.0 * positive(pre_act[:, run]) * hidden_grad).astype(BF16))
    pre_grad = [pre_grad] + [[route(p, k, 0) for p in pre_grad] for k in others]
    pre_grad = [jnp.concatenate(p, axis=1) for p in pre_grad]
    ins = [both(inputs, 0, tokens, 0)] + [x[:, -2 * block :] for x in gathered]
    w_up_g = jnp.concatenate([w_up, *after(w_up_parts, pre_grad[0])], axis=0)

    products = []
    for k in range(groups):
        products.append(rows_major(dot(pre_grad[k], w_up_g, 1, 1).astype(BF16)))
    pieces = []
    for k in range(groups):
        halves = products[k].reshape(n_tp // 2, 2, share, 2 * block)
        give = lax.dynamic_index_in_dim(halves, 1 - lane % 2, 1, keepdims=False)
        keep = lax.dynamic_index_in_dim(halves, lane % 2, 1, keepdims=False)
        taken = lax.ppermute(give, "tp", [(t, t ^ 1) for t in range(n_tp)])
        pieces.append((keep.astype(F32) + taken.astype(F32)).astype(BF16))
    same_parity = [list(range(c, n_tp, 2)) for c in (0, 1)]
    terms = jnp.concatenate(pieces, axis=1)
    terms = lax.all_to_all(terms, "tp", 0, 0, axis_index_groups=same_parity)
    terms = [terms[:, k * share : (k + 1) * share] for k in range(groups)]
    pieces = [jnp.sum(t.astype(F32), axis=0).astype(BF16) for t in terms]
    pieces = [pieces[0]] + [route(pieces[k], -k, 0) for k in others]
    ordered = []
    for h in range(groups):
        at = (h - group) % groups
        own, other = pieces[0][:, :block], pieces[0][:, block:]
        for k in others:
            own = jnp.where(at == k, pieces[k][:, :block], own)
            other = jnp.where(at == k, pieces[k][:, block:], other)
        ordered += [jnp.where(side == 0, own, other), jnp.where(side == 0, other, own)]
    grad_input = gather(jnp.concatenate(ordered, axis=1))

    hidden = [squared(a) for a in lax.optimization_barrier(([pre_act] + acts, pre_grad[0]))[0]]
    partial = summed([(h, c[:, block:]) for h, c in zip(hidden, cot)]).astype(BF16)
    kept = lax.optimization_barrier(summed([(h, c[:, :block]) for h, c in zip(hidden, cot)]))
    grad_down = kept + route(partial, 0, 1).astype(F32)

    partial = summed([(x[:, block:], p) for x, p in zip(ins, pre_grad)]).astype(BF16)
    kept = lax.optimization_barrier(summed([(x[:, :block], p) for x, p in zip(ins, pre_grad)]))
    received = route(partial, 0, 1)
    grad_up = kept + after(received, grad_input).astype(F32)
    return grad_input, grad_up, grad_down


def solution(mesh):
    n_fs, n_tp = mesh.shape["fs"], mesh.shape["tp"]
    in_specs = (P("fs", None), P("fs", "tp"), P("fs", None), P("fs", "tp"), P("tp", "fs"))
    out_specs = (P("fs", None), P("fs", "tp"), P("tp", "fs"))

    def on_device(*args):
        return body(*args, n_fs, n_tp)

    return jax.shard_map(
        on_device, mesh=mesh, in_specs=in_specs, out_specs=out_specs, check_vma=False
    )
```
